32 devices in a mesh: sp: 16 (over z, y, x), tp: 2 (over core).
Axes of the slice: x: 2, y: 2, z: 4, core: 2. Of those that a mesh axis runs over, the one named last changes fastest.
Arguments:
- acceptor_signal: bfloat16 [2048, 1024], P('sp', 'tp'), may hold values from -6 to 6
- address_entries: bfloat16 [2048, 1024], P('sp', 'tp'), may hold values from -6 to 6
- payload_entries: bfloat16 [2048, 1024], P('sp', 'tp'), may hold values from -6 to 6
- fading_logits: float32 [2048, 1024], P('sp', 'tp'), may hold values from -12 to -2
- learning_rate_logits: float32 [2048, 1024], P('sp', 'tp'), may hold values from -10 to 4
- exit_switch_entries: bfloat16 [2048, 1024], P('sp', 'tp'), may hold values from -6 to 6
- extra_reward_weights: float32 [1024], P('tp'), may hold values from -0.3 to 0.3
- subspace_rescale_weights: float32 [1024], P('tp'), may hold values from 0.1 to 1.9
- timemix_exit_weights: bfloat16 [1024, 2048], P('tp'), may hold values from -0.1875 to 0.1875
- skip_stream_arriving: bfloat16 [2048, 2048], P(('sp', 'tp')), may hold values from -6 to 6
- pointwise_block_scaling: float32 [2048], replicated, may hold values from 0.1 to 1.9
- switch_projection: bfloat16 [2048, 5632], P('sp', 'tp'), may hold values from -0.125 to 0.125
- widening_projection: bfloat16 [2048, 5632], P('sp', 'tp'), may hold values from -0.125 to 0.125
- switch_filter_coefficients: float32 [3, 5632], P(None, 'tp'), may hold values from -3.5 to 3.5
- narrowing_projection: bfloat16 [5632, 2048], P('tp', 'sp'), may hold values from -0.078125 to 0.078125
Outputs:
- layer_out: bfloat16 [2048, 2048], P(('sp', 'tp'))
The draws below stay inside these ranges and needn't reach their ends.
All inputs are finite; a program needn't handle non-finite values.
Results may differ from the reference program's by a relative error of at most 0.019.
Values may be sent and summed in bfloat16 or wider, within the bound.
A program may use at most 128 MiB of HBM per device.

```python
import jax
import jax.numpy as jnp
from jax import lax

D = 2048
HEADS = 16
SUBSPACE_WIDTH = 64
FF = 5632
TAPS = 3
TOK_DEV = 128
TOKENS = 2048
TIMEMIX_FEATURES = 1024
N_TP = 2


def head_kinds(key):
    drawn = jax.random.randint(jax.random.fold_in(key, 11), (HEADS,), 0, 10)
    slow = drawn < 5
    return jnp.repeat(slow, SUBSPACE_WIDTH)


def draw_fading_logits(key, part):
    slow = head_kinds(key)
    slow_base = 0.3 - jnp.log(TOKENS * 1.0)
    base = jnp.where(slow, slow_base, -3.4).astype(jnp.float32)
    offsets = jax.random.uniform(jax.random.fold_in(key, 21), (TOKENS // TOK_DEV, HEADS * SUBSPACE_WIDTH), jnp.float32, -0.7, 0.7)
    offsets = jnp.repeat(offsets, TOK_DEV, axis=0)
    noise = 0.3 * jax.random.normal(jax.random.fold_in(key, 31), (TOKENS, HEADS * SUBSPACE_WIDTH), jnp.float32)
    return jnp.clip(base[None, :] + offsets + noise, -12.0, -2.0)


def draw_learning_rate_logits(key, part):
    slow = head_kinds(key)
    slow_base = -1.0 - jnp.log(TOKENS / 64.0)
    base = jnp.where(slow, slow_base, 0.0).astype(jnp.float32)
    spread = jnp.where(slow, 0.7, 1.0).astype(jnp.float32)
    noise = jax.random.normal(jax.random.fold_in(key, 41), (TOKENS, HEADS * SUBSPACE_WIDTH), jnp.float32)
    return jnp.clip(base[None, :] + spread[None, :] * noise, -10.0, 4.0)


def block_levels(key, shape, pieces, least, top_value):
    def one(dim, shards_of):
        heights = jax.random.uniform(jax.random.fold_in(jax.random.fold_in(key, 6), dim), (shards_of,), jnp.float32, least / len(pieces), top_value / len(pieces))
        return jnp.repeat(jnp.exp(heights), shape[dim] // shards_of).reshape((-1,) + (1,) * (len(shape) - dim - 1))

    level = one(*pieces[0])
    for cut in pieces[1:]:
        level = level * one(*cut)
    return level


def gaussian(stream_key, dims, scale, reach, shards=(), held_as=jnp.bfloat16):
    values = scale * jax.random.normal(stream_key, dims, jnp.float32)
    if shards:
        values = values * block_levels(stream_key, dims, shards, -0.22, 0.18)
    return jnp.clip(values, -reach, reach).astype(held_as)


def setup_inputs(seed: int = 0) -> dict:
    streams_of = jax.random.split(jax.random.key(seed), 16)
    acceptor_signal = gaussian(streams_of[0], (TOKENS, TIMEMIX_FEATURES), 1.0, 6.0, ((0, 16), (1, 2)))
    address_entries = gaussian(streams_of[1], (TOKENS, TIMEMIX_FEATURES), 1.0, 6.0, ((0, 16), (1, 2)))
    payload_entries = gaussian(streams_of[2], (TOKENS, TIMEMIX_FEATURES), 1.0, 6.0, ((0, 16), (1, 2)))
    fading_logits = draw_fading_logits(jax.random.fold_in(streams_of[15], 71), 0)
    learning_rate_logits = draw_learning_rate_logits(jax.random.fold_in(streams_of[15], 71), 0)
    exit_switch_entries = gaussian(streams_of[5], (TOKENS, TIMEMIX_FEATURES), 1.0, 6.0, ((0, 16), (1, 2)))
    extra_reward_weights = gaussian(streams_of[6], (TIMEMIX_FEATURES,), 0.05, 0.3, ((0, 2),), jnp.float32)
    subspace_rescale_weights = jnp.clip(1.0 + 0.18 * jax.random.normal(streams_of[7], (TIMEMIX_FEATURES,), jnp.float32), 0.1, 1.9)
    timemix_exit_weights = gaussian(streams_of[8], (TIMEMIX_FEATURES, D), TIMEMIX_FEATURES ** -0.5, 0.1875, ((0, 2),))
    skip_stream_arriving = gaussian(streams_of[9], (TOKENS, D), 1.0, 6.0, ((0, 32),))
    pointwise_block_scaling = jnp.clip(1.0 + 0.18 * jax.random.normal(streams_of[10], (D,), jnp.float32), 0.1, 1.9)
    switch_projection = gaussian(streams_of[11], (D, FF), D ** -0.5, 0.125, ((0, 16), (1, 2)))
    widening_projection = gaussian(streams_of[12], (D, FF), D ** -0.5, 0.125, ((0, 16), (1, 2)))
    switch_filter_coefficients = gaussian(streams_of[13], (TAPS, FF), TAPS ** -0.5, 3.5, ((1, 2),), jnp.float32)
    narrowing_projection = gaussian(streams_of[14], (FF, D), FF ** -0.5, 0.078125, ((0, 2), (1, 16)))
    return dict(acceptor_signal=acceptor_signal, address_entries=address_entries, payload_entries=payload_entries, fading_logits=fading_logits, learning_rate_logits=learning_rate_logits, exit_switch_entries=exit_switch_entries, extra_reward_weights=extra_reward_weights, subspace_rescale_weights=subspace_rescale_weights, timemix_exit_weights=timemix_exit_weights, skip_stream_arriving=skip_stream_arriving, pointwise_block_scaling=pointwise_block_scaling, switch_projection=switch_projection, widening_projection=widening_projection, switch_filter_coefficients=switch_filter_coefficients, narrowing_projection=narrowing_projection)


group_eps = 0.00064
norm_eps = 1e-06
highest = lax.Precision.HIGHEST

def by_heads(array):
    return array.astype(jnp.float32).reshape(array.shape[0], -1, SUBSPACE_WIDTH)

def mechanism_inputs(acceptor_signal, address_entries, payload_entries, fading_logits, learning_rate_logits):
    acceptor_entries = by_heads(acceptor_signal)
    address_mapped = by_heads(address_entries)
    payload_mapped = by_heads(payload_entries)
    log_rate = -jax.nn.softplus(-fading_logits) - 0.5
    fading = by_heads(jnp.exp(-jnp.exp(log_rate)))
    erase_rate = by_heads(jax.nn.sigmoid(learning_rate_logits))
    length = jnp.sqrt(lax.optimization_barrier(jnp.sum(address_mapped * address_mapped, axis=-1, keepdims=True)))
    unit_key = address_mapped / jnp.maximum(length, 1.0)
    return (acceptor_entries, address_mapped, payload_mapped, fading, -unit_key, unit_key * erase_rate)

def subspace_outcomes(acceptor_entries, address_mapped, payload_mapped, closing_memory, subspace_rescale_weights, extra_reward_weights, exit_switch_entries):
    centred = closing_memory - lax.optimization_barrier(jnp.mean(closing_memory, axis=-1, keepdims=True))
    rescaled_arguments = centred * lax.rsqrt(lax.optimization_barrier(jnp.mean(centred * centred, axis=-1, keepdims=True)) + group_eps)
    scaling_fetch = subspace_rescale_weights.reshape(-1, SUBSPACE_WIDTH)
    extra_reward_fetch = extra_reward_weights.reshape(-1, SUBSPACE_WIDTH)
    present_extra_reward = lax.optimization_barrier(jnp.sum(acceptor_entries * address_mapped * extra_reward_fetch, axis=-1, keepdims=True)) * payload_mapped
    timemix_product = rescaled_arguments * scaling_fetch + present_extra_reward
    timemix_product = timemix_product.reshape(timemix_product.shape[0], -1) * exit_switch_entries.astype(jnp.float32)
    return timemix_product.astype(jnp.bfloat16)

def token_step(state, sublevel_arguments):
    acceptor_entries, address_mapped, payload_mapped, fading, erase_dir, erase_amt = sublevel_arguments
    along = jnp.einsum('hij,hj->hi', state, erase_dir, precision=highest)
    state = state * fading[:, None, :] + along[:, :, None] * erase_amt[:, None, :] + payload_mapped[:, :, None] * address_mapped[:, None, :]
    return (state, jnp.einsum('hij,hj->hi', state, acceptor_entries, precision=highest))

def grouped_product(left, right, groups):
    width = left.shape[1] // groups
    total = jnp.zeros((left.shape[0], right.shape[1]), jnp.float32)
    for group in range(groups):
        part = jnp.dot(left[:, group * width:(group + 1) * width], right[group * width:(group + 1) * width], preferred_element_type=jnp.float32)
        rounded = lax.optimization_barrier(part.astype(jnp.bfloat16))
        total = total + rounded.astype(jnp.float32)
    return total

def reference(acceptor_signal, address_entries, payload_entries, fading_logits, learning_rate_logits, exit_switch_entries, extra_reward_weights, subspace_rescale_weights, timemix_exit_weights, skip_stream_arriving, pointwise_block_scaling, switch_projection, widening_projection, switch_filter_coefficients, narrowing_projection):
    sublevel_arguments = mechanism_inputs(acceptor_signal, address_entries, payload_entries, fading_logits, learning_rate_logits)
    head_count = sublevel_arguments[0].shape[1]
    initial = jnp.zeros((head_count, SUBSPACE_WIDTH, SUBSPACE_WIDTH), jnp.float32)
    _, closing_memory = lax.scan(token_step, initial, sublevel_arguments)
    timemix_product = subspace_outcomes(sublevel_arguments[0], sublevel_arguments[1], sublevel_arguments[2], closing_memory, subspace_rescale_weights, extra_reward_weights, exit_switch_entries)
    attended = grouped_product(timemix_product, timemix_exit_weights, N_TP)
    hidden_res = skip_stream_arriving.astype(jnp.float32) + attended
    rescaled_arguments = hidden_res * lax.rsqrt(lax.optimization_barrier(jnp.mean(hidden_res * hidden_res, axis=-1, keepdims=True)) + norm_eps) * pointwise_block_scaling
    rescaled_arguments = rescaled_arguments.astype(jnp.bfloat16)
    gate_pre = jnp.dot(rescaled_arguments, switch_projection, preferred_element_type=jnp.float32).astype(jnp.bfloat16)
    up_part = jnp.dot(rescaled_arguments, widening_projection, preferred_element_type=jnp.float32).astype(jnp.bfloat16)
    taps = switch_filter_coefficients.shape[0]
    padded = jnp.pad(gate_pre.astype(jnp.float32), ((taps - 1, 0), (0, 0)))
    length = gate_pre.shape[0]
    conv_out = jnp.zeros(gate_pre.shape, jnp.float32)
    for tap in range(taps):
        conv_out = conv_out + switch_filter_coefficients[tap] * padded[tap:tap + length]
    hidden = (jax.nn.silu(conv_out) * up_part.astype(jnp.float32)).astype(jnp.bfloat16)
    projected = grouped_product(hidden, narrowing_projection, N_TP)
    return (hidden_res + projected).astype(jnp.bfloat16)
```

```python
import functools

import jax
import jax.numpy as jnp
from jax import lax
from jax.experimental import pallas as pl
from jax.experimental.pallas import tpu as pltpu
from jax.sharding import Mesh, PartitionSpec as P

WIDTH = 64
GROUP = 4
group_eps = 0.00064
norm_eps = 1e-06
f32, bf16 = jnp.float32, jnp.bfloat16
NN, NT, TN = ((1,), (0,)), ((1,), (1,)), ((0,), (0,))


def split(a):
    high = a.astype(bf16)
    return high, (a - high.astype(f32)).astype(bf16)


def dot(a, b, dims=NN):
    return lax.dot_general(a, b, (dims, ((), ())), preferred_element_type=f32)


def dot3(a, b, dims=NN):
    (ah, al), (bh, bl) = a, b
    return dot(ah, bh, dims) + (dot(ah, bl, dims) + dot(al, bh, dims))


def chunk_kernel(r_ref, k_ref, v_ref, x_ref, l_ref, q_ref, o_ref, m_ref):
    tokens, lanes = r_ref.shape
    row = lax.broadcasted_iota(jnp.int32, (tokens, tokens), 0)
    col = lax.broadcasted_iota(jnp.int32, (tokens, tokens), 1)
    log_decay = -jax.nn.sigmoid(x_ref[...]) * jnp.exp(jnp.asarray(-0.5, f32))
    ones = (row >= col).astype(bf16)
    d0, rest = split(log_decay)[0], log_decay
    rest = log_decay - d0.astype(f32)
    d1, d2 = split(rest)
    running = dot(ones, d0) + (dot(ones, d1) + dot(ones, d2))
    decay = jnp.exp(running)
    before = jnp.exp(running - log_decay)
    inverse = jnp.exp(-running)
    rate = jax.nn.sigmoid(l_ref[...])
    r_all, k_all, v_all = (a[...].astype(f32) for a in (r_ref, k_ref, v_ref))
    k_hat_all = k_all * inverse
    r_hat_all = r_all * decay
    for head in range(lanes // WIDTH):
        cut = slice(head * WIDTH, (head + 1) * WIDTH)
        k = k_all[:, cut]
        length = jnp.sqrt(jnp.sum(k * k, axis=-1, keepdims=True))
        unit = k / jnp.maximum(length, 1.0)
        a_hat = -unit * before[:, cut]
        b_hat = unit * rate[:, cut] * inverse[:, cut]
        k_hat, r_hat = k_hat_all[:, cut], r_hat_all[:, cut]
        v = v_ref[:, cut]
        bk = split(jnp.concatenate([b_hat, k_hat], axis=0))
        both = dot3(split(jnp.concatenate([a_hat, r_hat], axis=0)), bk, NT)
        erase = jnp.where(row > col, both[:tokens, :tokens], 0.0)
        write = jnp.where(row > col, both[:tokens, tokens:], 0.0)
        out_erase = jnp.where(row >= col, both[tokens:, :tokens], 0.0)
        out_write = jnp.where(row >= col, both[tokens:, tokens:], 0.0)
        solved = (row == col).astype(f32)
        block = 1
        while block < tokens:
            off = (row // block == col // block + 1) & (row // (2 * block) == col // (2 * block))
            part = jnp.where(off, erase, 0.0)
            if block == 1:
                solved = solved + part
            else:
                pieces = split(solved)
                solved = solved + dot3(split(dot3(pieces, split(part))), pieces)
            block *= 2
        wh, wl = split(write)
        seen = jnp.concatenate([a_hat, dot(wh, v) + dot(wl, v)], axis=1)
        kept = dot3(split(solved), split(seen))
        kept_pieces = split(kept)
        oh, ol = split(out_write)
        out = dot3(split(out_erase), kept_pieces) + jnp.concatenate(
            [r_hat, dot(oh, v) + dot(ol, v)], axis=1
        )
        q_ref[:, cut] = out[:, :WIDTH]
        o_ref[:, cut] = out[:, WIDTH:]
        moved = dot3(kept_pieces, tuple(p[:tokens] for p in bk), TN)
        kh, kl = (p[tokens:] for p in bk)
        stored = dot(v, kh, TN) + dot(v, kl, TN)
        eye = (row == col)[:WIDTH, :WIDTH].astype(f32)
        last = decay[tokens - 1 :, cut]
        m_ref[head] = jnp.concatenate(
            [(moved[:WIDTH] + eye) * last, (moved[WIDTH:] + stored) * last], axis=1
        ).astype(bf16)


def chunk(r, k, v, x, l):
    tokens, channels = r.shape
    pair = 2 * WIDTH
    heads = channels // WIDTH
    block = pl.BlockSpec((tokens, pair), lambda i: (0, i))
    return pl.pallas_call(
        chunk_kernel,
        grid=(channels // pair,),
        out_shape=(
            jax.ShapeDtypeStruct((tokens, channels), f32),
            jax.ShapeDtypeStruct((tokens, channels), f32),
            jax.ShapeDtypeStruct((heads, WIDTH, pair), bf16),
        ),
        in_specs=[block] * 5,
        out_specs=(block, block, pl.BlockSpec((2, WIDTH, pair), lambda i: (i, 0, 0))),
        cost_estimate=pl.CostEstimate(
            flops=heads * 200_000_000, bytes_accessed=tokens * channels * 22, transcendentals=0
        ),
        name="chunk",
    )(r, k, v, x, l)


def finish_kernel(me_ref, maps_ref, q_ref, o_ref, r_ref, k_ref, v_ref, g_ref, e_ref, s_ref, w_ref, out_ref, mixed):
    heads = maps_ref.shape[1]

    def step(i, states):
        following = []
        for head in range(heads):
            joined = maps_ref[i, head]
            move, add = joined[:, :WIDTH], joined[:, WIDTH:]
            high, low = split(states[head])
            following.append(dot(high, move) + dot(low, move) + add.astype(f32))
        return tuple(following)

    start = tuple(jnp.zeros((WIDTH, WIDTH), f32) for _ in range(heads))
    states = lax.fori_loop(0, me_ref[0], step, start)
    for head in range(heads):
        cut = slice(head * WIDTH, (head + 1) * WIDTH)
        o = o_ref[:, cut] + dot3(split(q_ref[:, cut]), split(states[head]), NT)
        centred = o - jnp.mean(o, axis=-1, keepdims=True)
        scaled = centred * lax.rsqrt(jnp.mean(centred * centred, axis=-1, keepdims=True) + group_eps)
        r, k, v, g = (a[:, cut].astype(f32) for a in (r_ref, k_ref, v_ref, g_ref))
        bonus = jnp.sum(r * k * e_ref[:, cut], axis=-1, keepdims=True) * v
        mixed[:, cut] = ((scaled * s_ref[:, cut] + bonus) * g).astype(bf16)
    out_ref[...] = dot(mixed[...], w_ref[...]).astype(bf16)


def finish(me, maps, q, o, r, k, v, g, extra, scale, weights):
    tokens, channels = r.shape
    vmem = pl.BlockSpec(memory_space=pltpu.VMEM)
    return pl.pallas_call(
        finish_kernel,
        out_shape=jax.ShapeDtypeStruct((tokens, weights.shape[1]), bf16),
        in_specs=[pl.BlockSpec(memory_space=pltpu.SMEM)] + [vmem] * 10,
        out_specs=vmem,
        scratch_shapes=[pltpu.VMEM((tokens, channels), bf16)],
        cost_estimate=pl.CostEstimate(
            flops=2_000_000_000, bytes_accessed=4_000_000, transcendentals=0
        ),
        name="finish",
    )(me, maps, q, o, r, k, v, g, extra[None], scale[None], weights)


def body(
    r, k, v, x, l, g, extra, scale, exit_weights, skip, gain, gate_w, up_w, taps_w, down_w
):
    token_count = r.shape[0]
    place = lax.axis_index(("z", "p"))

    gate_up = jnp.concatenate([gate_w, up_w], axis=0).reshape((2,) + gate_w.shape)
    gate_up = lax.all_to_all(gate_up, "p", split_axis=2, concat_axis=1, tiled=True)
    down_part = lax.all_to_all(down_w, "p", split_axis=0, concat_axis=1, tiled=True)

    q, o, maps = chunk(r, k, v, x, l)
    maps = lax.all_gather(maps, ("z", "p"))
    gate_full = lax.all_gather(gate_up[0], "z", axis=0, tiled=True)
    up_full = lax.all_gather(gate_up[1], "z", axis=0, tiled=True)
    down_full = lax.all_gather(down_part, "z", axis=1, tiled=True)
    partial = finish(place[None].astype(jnp.int32), maps, q, o, r, k, v, g, extra, scale, exit_weights)
    attended = lax.psum_scatter(partial, "t", scatter_dimension=0, tiled=True).astype(f32)
    hidden_res = skip.astype(f32) + attended
    normed = (
        hidden_res
        * lax.rsqrt(jnp.mean(hidden_res * hidden_res, axis=-1, keepdims=True) + norm_eps)
        * gain
    ).astype(bf16)
    rows = lax.all_gather(normed, ("p", "t"), axis=0, tiled=True)
    gate_pre = jnp.dot(rows, gate_full, preferred_element_type=f32).astype(bf16)
    count, taps = rows.shape[0], taps_w.shape[0]
    groups = lax.axis_size("z")
    tail = lax.ppermute(gate_pre[count - taps + 1 :], "z", [(i, i + 1) for i in range(groups - 1)])
    up_part = jnp.dot(rows, up_full, preferred_element_type=f32).astype(bf16)
    units = gate_pre.shape[1]
    own_taps = lax.dynamic_slice_in_dim(taps_w, lax.axis_index("p") * units, units, 1)
    extended = jnp.concatenate([tail, gate_pre], axis=0).astype(f32)
    conv_out = jnp.zeros(gate_pre.shape, f32)
    for tap in range(taps):
        conv_out = conv_out + own_taps[tap] * extended[tap : tap + count]
    hidden = (jax.nn.silu(conv_out) * up_part.astype(f32)).astype(bf16)
    projected = lax.psum_scatter(
        jnp.dot(hidden, down_full, preferred_element_type=f32).astype(bf16),
        ("p", "t"),
        scatter_dimension=0,
        tiled=True,
    ).astype(f32)
    return (hidden_res + projected).astype(bf16)


def solution(mesh):
    names = mesh.axis_names
    spread, wide = mesh.shape[names[0]], mesh.shape[names[1]]
    group = GROUP if spread % GROUP == 0 else 1
    fine = Mesh(mesh.devices.reshape(spread // group, group, wide), ("z", "p", "t"))
    sp = ("z", "p")
    both = P(sp, "t")
    return jax.shard_map(
        body,
        mesh=fine,
        in_specs=(
            both, both, both, both, both, both,
            P("t"), P("t"), P("t", None),
            P(("z", "p", "t"), None), P(),
            both, both, P(None, "t"), P("t", sp),
        ),
        out_specs=P(("z", "p", "t"), None),
        check_vma=False,
    )
```

```python
import functools

import jax
import jax.numpy as jnp
from jax import lax
from jax.experimental import pallas as pl
from jax.experimental.pallas import tpu as pltpu
from jax.sharding import Mesh, PartitionSpec as P

WIDTH = 64
GROUP = 4
group_eps = 0.00064
norm_eps = 1e-06
f32, bf16 = jnp.float32, jnp.bfloat16
NN, NT, TN = ((1,), (0,)), ((1,), (1,)), ((0,), (0,))


def split(a):
    high = a.astype(bf16)
    return high, (a - high.astype(f32)).astype(bf16)


def dot(a, b, dims=NN):
    return lax.dot_general(a, b, (dims, ((), ())), preferred_element_type=f32)


def dot3(a, b, dims=NN):
    (ah, al), (bh, bl) = a, b
    return dot(ah, bh, dims) + (dot(ah, bl, dims) + dot(al, bh, dims))


MESH = pl.DeviceIdType.MESH


def others(axis):
    size, me = lax.axis_size(axis), lax.axis_index(axis)
    return [(lax.rem(me + d, size), lax.rem(me + size - d, size)) for d in range(1, size)]


def peers(kinds):
    found = []
    for kind in kinds:
        if kind[0] == "oa":
            found += outer_peers()[0]
        else:
            found += [{kind[0]: to} for to, _ in others(kind[0])]
    return found


def outer_peers():
    count, size = lax.axis_size("o") * lax.axis_size("a"), lax.axis_size("a")
    me = lax.axis_index("o") * size + lax.axis_index("a")
    to, come = [], []
    for d in range(1, count):
        there = lax.rem(me + d, count)
        to.append({"o": there // size, "a": lax.rem(there, size)})
        come.append(lax.rem(me + count - d, count))
    return to, come, me


def greet(kinds):
    barrier = pltpu.get_barrier_semaphore()
    who = peers(kinds)
    for device in who:
        pl.semaphore_signal(barrier, inc=1, device_id=device, device_id_type=MESH)
    pl.semaphore_wait(barrier, len(who))


def remote(src, dst, send, recv, device):
    return pltpu.make_async_remote_copy(
        src_ref=src, dst_ref=dst, send_sem=send, recv_sem=recv, device_id=device, device_id_type=MESH
    )


def exchange(sources, targets, sends, recvs, local, begin):
    me = lax.axis_index("a")
    for n, (src, dst) in enumerate(zip(sources, targets)):
        own = pltpu.make_async_copy(src.at[me], dst.at[me], local.at[n])
        if begin:
            own.start()
        for d, (to, come) in enumerate(others("a")):
            out = remote(src.at[to], dst.at[me], sends.at[n, d], recvs.at[n, me], {"a": to})
            if begin:
                out.start()
            else:
                out.wait_send()
                remote(src.at[to], dst.at[come], sends.at[n, d], recvs.at[n, come], {"a": to}).wait_recv()
        if not begin:
            own.wait()


def chunk_kernel(r_ref, k_ref, v_ref, x_ref, l_ref, gate, up, down, q_ref, o_ref, m_ref, gate_out, up_out, down_out, sends, recvs, local):
    swap = functools.partial(exchange, (gate, up, down), (gate_out, up_out, down_out), sends, recvs, local)

    @pl.when(pl.program_id(0) == 0)
    def _():
        greet([("a",)])
        swap(True)

    tokens, lanes = r_ref.shape
    row = lax.broadcasted_iota(jnp.int32, (tokens, tokens), 0)
    col = lax.broadcasted_iota(jnp.int32, (tokens, tokens), 1)
    log_decay = -jax.nn.sigmoid(x_ref[...]) * jnp.exp(jnp.asarray(-0.5, f32))
    ones = (row >= col).astype(bf16)
    d0, rest = split(log_decay)[0], log_decay
    rest = log_decay - d0.astype(f32)
    d1, d2 = split(rest)
    running = dot(ones, d0) + (dot(ones, d1) + dot(ones, d2))
    decay = jnp.exp(running)
    before = jnp.exp(running - log_decay)
    inverse = jnp.exp(-running)
    rate = jax.nn.sigmoid(l_ref[...])
    r_all, k_all, v_all = (a[...].astype(f32) for a in (r_ref, k_ref, v_ref))
    k_hat_all = k_all * inverse
    r_hat_all = r_all * decay
    for head in range(lanes // WIDTH):
        cut = slice(head * WIDTH, (head + 1) * WIDTH)
        k = k_all[:, cut]
        length = jnp.sqrt(jnp.sum(k * k, axis=-1, keepdims=True))
        unit = k / jnp.maximum(length, 1.0)
        a_hat = -unit * before[:, cut]
        b_hat = unit * rate[:, cut] * inverse[:, cut]
        k_hat, r_hat = k_hat_all[:, cut], r_hat_all[:, cut]
        v = v_ref[:, cut]
        bk = split(jnp.concatenate([b_hat, k_hat], axis=0))
        both = dot3(split(jnp.concatenate([a_hat, r_hat], axis=0)), bk, NT)
        erase = jnp.where(row > col, both[:tokens, :tokens], 0.0)
        write = jnp.where(row > col, both[:tokens, tokens:], 0.0)
        out_erase = jnp.where(row >= col, both[tokens:, :tokens], 0.0)
        out_write = jnp.where(row >= col, both[tokens:, tokens:], 0.0)
        solved = (row == col).astype(f32)
        block = 1
        while block < tokens:
            off = (row // block == col // block + 1) & (row // (2 * block) == col // (2 * block))
            part = jnp.where(off, erase, 0.0)
            if block == 1:
                solved = solved + part
            else:
                pieces = split(solved)
                solved = solved + dot3(split(dot3(pieces, split(part))), pieces)
            block *= 2
        wh, wl = split(write)
        seen = jnp.concatenate([a_hat, dot(wh, v) + dot(wl, v)], axis=1)
        kept = dot3(split(solved), split(seen))
        kept_pieces = split(kept)
        oh, ol = split(out_write)
        out = dot3(split(out_erase), kept_pieces) + jnp.concatenate(
            [r_hat, dot(oh, v) + dot(ol, v)], axis=1
        )
        q_ref[:, cut] = out[:, :WIDTH]
        o_ref[:, cut] = out[:, WIDTH:]
        moved = dot3(kept_pieces, tuple(p[:tokens] for p in bk), TN)
        kh, kl = (p[tokens:] for p in bk)
        stored = dot(v, kh, TN) + dot(v, kl, TN)
        eye = (row == col)[:WIDTH, :WIDTH].astype(f32)
        last = decay[tokens - 1 :, cut]
        m_ref[head] = jnp.concatenate(
            [(moved[:WIDTH] + eye) * last, (moved[WIDTH:] + stored) * last], axis=1
        ).astype(bf16)

    @pl.when(pl.program_id(0) == pl.num_programs(0) - 1)
    def _():
        swap(False)


def chunk(r, k, v, x, l, gate, up, down):
    tokens, channels = r.shape
    pair = 2 * WIDTH
    heads = channels // WIDTH
    size = gate.shape[0]
    block = pl.BlockSpec((tokens, pair), lambda i: (0, i))
    hbm = pl.BlockSpec(memory_space=pltpu.HBM)
    return pl.pallas_call(
        chunk_kernel,
        grid=(channels // pair,),
        out_shape=(
            jax.ShapeDtypeStruct((tokens, channels), f32),
            jax.ShapeDtypeStruct((tokens, channels), f32),
            jax.ShapeDtypeStruct((heads, WIDTH, pair), bf16),
        )
        + tuple(jax.ShapeDtypeStruct(w.shape, bf16) for w in (gate, up, down)),
        in_specs=[block] * 5 + [hbm] * 3,
        out_specs=(block, block, pl.BlockSpec((2, WIDTH, pair), lambda i: (i, 0, 0)), hbm, hbm, hbm),
        scratch_shapes=[
            pltpu.SemaphoreType.DMA((3, size)),
            pltpu.SemaphoreType.DMA((3, size)),
            pltpu.SemaphoreType.DMA((3,)),
        ],
        compiler_params=pltpu.CompilerParams(collective_id=0, has_side_effects=True),
        cost_estimate=pl.CostEstimate(
            flops=heads * 200_000_000, bytes_accessed=tokens * channels * 22, transcendentals=0
        ),
        name="chunk",
    )(r, k, v, x, l, gate, up, down)


def finish_kernel(
    m_ref, q_ref, o_ref, r_ref, k_ref, v_ref, g_ref, e_ref, s_ref, w_ref, skip_ref, gain_ref,
    rows_ref, res_ref,
    near, total, far, mixed, partial, parts, near_s, near_r, far_s, far_r, part_s, part_r, row_s, row_r, pass_s,
):
    heads = m_ref.shape[0]
    side, across = lax.axis_size("b"), far.shape[0]
    b, a, t = lax.axis_index("b"), lax.axis_index("a"), lax.axis_index("t")
    wide = lax.axis_size("t")
    greet([("b",), ("oa",), ("t",)])

    sent = []
    for d, (to, come) in enumerate(others("b")):
        copy = remote(m_ref, near.at[b], near_s.at[d], near_r.at[b], {"b": to})
        copy.start()
        sent.append(copy)
    for to, come in others("b"):
        remote(m_ref, near.at[come], near_s.at[0], near_r.at[come], {"b": to}).wait_recv()
    near[b] = m_ref[...]
    eye = (
        lax.broadcasted_iota(jnp.int32, (2 * WIDTH, WIDTH), 0)
        == lax.broadcasted_iota(jnp.int32, (2 * WIDTH, WIDTH), 1)
    ).astype(f32)
    befores = [eye] * heads
    for head in range(heads):
        running = None
        for i in range(side):
            joined = near[i, head]
            move, add = joined[:, :WIDTH], joined[:, WIDTH:]
            if running is None:
                running = jnp.concatenate([move, add], axis=0).astype(f32)
            else:
                befores[head] = jnp.where(b == i, running, befores[head])
                high, low = split(running)
                running = dot(high, move) + dot(low, move)
                running = running + jnp.concatenate(
                    [jnp.zeros((WIDTH, WIDTH), f32), add.astype(f32)], axis=0
                )
        total[head] = jnp.concatenate([running[:WIDTH], running[WIDTH:]], axis=1).astype(bf16)

    to_outer, come_outer, outer = outer_peers()
    for d, device in enumerate(to_outer):
        copy = remote(total, far.at[outer], far_s.at[d], far_r.at[outer], device)
        copy.start()
        sent.append(copy)
    for come, device in zip(come_outer, to_outer):
        remote(total, far.at[come], far_s.at[0], far_r.at[come], device).wait_recv()
    far[outer] = total[...]
    for head in range(heads):
        state = jnp.zeros((WIDTH, WIDTH), f32)
        for i in range(across - 1):
            joined = far[i, head]
            high, low = split(state)
            following = dot(high, joined[:, :WIDTH]) + dot(low, joined[:, :WIDTH])
            state = jnp.where(i < outer, following + joined[:, WIDTH:].astype(f32), state)
        state = dot3(split(state), split(befores[head][:WIDTH])) + befores[head][WIDTH:]
        cut = slice(head * WIDTH, (head + 1) * WIDTH)
        o = o_ref[:, cut] + dot3(split(q_ref[:, cut]), split(state), NT)
        centred = o - jnp.mean(o, axis=-1, keepdims=True)
        scaled = centred * lax.rsqrt(jnp.mean(centred * centred, axis=-1, keepdims=True) + group_eps)
        r, k, v, g = (x[:, cut].astype(f32) for x in (r_ref, k_ref, v_ref, g_ref))
        bonus = jnp.sum(r * k * e_ref[:, cut], axis=-1, keepdims=True) * v
        mixed[:, cut] = ((scaled * s_ref[:, cut] + bonus) * g).astype(bf16)

    own = skip_ref.shape[0]
    product = dot(mixed[...], w_ref[...]).astype(bf16)
    for n in range(wide):
        partial[n] = product[n * own : (n + 1) * own]
    for d, (to, come) in enumerate(others("t")):
        copy = remote(partial.at[to], parts.at[t], part_s.at[d], part_r.at[t], {"t": to})
        copy.start()
        sent.append(copy)
    for to, come in others("t"):
        remote(partial.at[to], parts.at[come], part_s.at[0], part_r.at[come], {"t": to}).wait_recv()
    parts[t] = partial[t]
    hidden_res = skip_ref[...].astype(f32)
    attended = parts[0].astype(f32)
    for n in range(1, wide):
        attended = attended + parts[n].astype(f32)
    hidden_res = hidden_res + attended
    res_ref[...] = hidden_res
    normed = (
        hidden_res
        * lax.rsqrt(jnp.mean(hidden_res * hidden_res, axis=-1, keepdims=True) + norm_eps)
        * gain_ref[...]
    )
    normed = normed.astype(bf16)
    outers, along = lax.axis_size("o"), lax.axis_size("a")
    piece = normed.shape[1] // (outers * along * side)
    starts = [((i * along + j) * side + n) * piece for i in range(outers) for n in range(side) for j in range(along)]
    rows_ref[a, t] = jnp.concatenate([normed[:, at : at + piece] for at in starts], axis=1)

    def give(slot, send, device):
        copy = remote(rows_ref.at[slot, t], rows_ref.at[slot, t], send, row_r.at[slot, t], device)
        copy.start()
        sent.append(copy)

    for d, (to, come) in enumerate(others("a")):
        give(a, row_s.at[d], {"a": to})
    for d, (to, come) in enumerate(others("t")):
        give(a, pass_s.at[0, d], {"t": to})
    for d, (to, come) in enumerate(others("a")):
        mine = rows_ref.at[come, t]
        remote(mine, mine, row_s.at[0], row_r.at[come, t], {"a": to}).wait_recv()
        for f, (fro, _) in enumerate(others("t")):
            give(come, pass_s.at[d + 1, f], {"t": fro})
    for i in range(lax.axis_size("a")):
        for to, come in others("t"):
            theirs = rows_ref.at[i, come]
            remote(theirs, theirs, row_s.at[0], row_r.at[i, come], {"t": to}).wait_recv()
    for copy in sent:
        copy.wait_send()


def finish(m, q, o, r, k, v, g, extra, scale, weights, skip, gain):
    tokens, channels = r.shape
    own, model = skip.shape
    side, along, wide = (lax.axis_size(x) for x in ("b", "a", "t"))
    across = lax.axis_size("o") * along
    vmem = pl.BlockSpec(memory_space=pltpu.VMEM)
    dma = pltpu.SemaphoreType.DMA
    return pl.pallas_call(
        finish_kernel,
        out_shape=(
            jax.ShapeDtypeStruct((along, wide, own, model), bf16),
            jax.ShapeDtypeStruct((own, model), f32),
        ),
        in_specs=[vmem] * 12,
        out_specs=(vmem, vmem),
        scratch_shapes=[
            pltpu.VMEM((side,) + m.shape, bf16),
            pltpu.VMEM(m.shape, bf16),
            pltpu.VMEM((across,) + m.shape, bf16),
            pltpu.VMEM((tokens, channels), bf16),
            pltpu.VMEM((wide, own, model), bf16),
            pltpu.VMEM((wide, own, model), bf16),
            dma((side,)), dma((side,)), dma((across,)), dma((across,)),
            dma((wide,)), dma((wide,)), dma((along,)), dma((along, wide)), dma((along, wide)),
        ],
        compiler_params=pltpu.CompilerParams(collective_id=1, has_side_effects=True),
        cost_estimate=pl.CostEstimate(
            flops=20_000_000_000, bytes_accessed=4_000_000, transcendentals=0
        ),
        name="finish",
    )(m, q, o, r, k, v, g, extra[None], scale[None], weights, skip, gain[None])


def body(
    r, k, v, x, l, g, extra, scale, exit_weights, skip, gain, gate_w, up_w, taps_w, down_w
):
    tokens = r.shape[0]
    along, side = lax.axis_size("a"), lax.axis_size("b")
    outer = lax.axis_size("o")
    piece = gate_w.shape[0]
    units = gate_w.shape[1] // along

    def by_owner(w):
        return jnp.moveaxis(w.reshape(piece, along, units), 1, 0)

    q, o, m, gate_part, up_part, down_part = chunk(
        r, k, v, x, l, by_owner(gate_w), by_owner(up_w), down_w.reshape(along, units, piece)
    )
    gate_full = lax.all_gather(gate_part, ("o", "b"), axis=0, tiled=True)
    up_full = lax.all_gather(up_part, ("o", "b"), axis=0, tiled=True)
    down_full = lax.all_gather(down_part, ("o", "b"), axis=0, tiled=True)
    rows, hidden_res = finish(
        m, q, o, r, k, v, g, extra, scale, exit_weights, skip, gain
    )
    rows = rows.reshape(along * tokens, -1)
    model = rows.shape[1]
    gate_full, up_full = gate_full.reshape(model, units), up_full.reshape(model, units)
    gate_pre = jnp.dot(rows, gate_full, preferred_element_type=f32).astype(bf16)
    gate_pre = gate_pre.reshape(along, tokens, units)
    reach = taps_w.shape[0] - 1
    tail = gate_pre[:, tokens - reach :]
    tail = lax.ppermute(tail, "b", [(i, (i + 1) % side) for i in range(side)])
    if outer > 1:
        first = lax.ppermute(tail[-1:], "o", [(i, i + 1) for i in range(outer - 1)])
    else:
        first = jnp.zeros_like(tail[:1])
    later = jnp.concatenate([first, tail[:-1]], axis=0)
    tail = jnp.where(lax.axis_index("b") == 0, later, tail)
    up_out = jnp.dot(rows, up_full, preferred_element_type=f32).astype(bf16)
    own_taps = lax.dynamic_slice_in_dim(taps_w, lax.axis_index("a") * units, units, 1)
    extended = jnp.concatenate([tail, gate_pre], axis=1).astype(f32)
    conv_out = jnp.zeros(gate_pre.shape, f32)
    for tap in range(reach + 1):
        conv_out = conv_out + own_taps[tap] * extended[:, tap : tap + tokens]
    hidden = (jax.nn.silu(conv_out).reshape(up_out.shape) * up_out.astype(f32)).astype(bf16)
    down_full = jnp.moveaxis(down_full.reshape(outer, side, along, units, piece), 3, 0)
    down_full = jnp.swapaxes(down_full, 2, 3).reshape(units, model)
    projected = lax.psum_scatter(
        jnp.dot(hidden, down_full, preferred_element_type=f32).astype(bf16),
        ("a", "t"),
        scatter_dimension=0,
        tiled=True,
    ).astype(f32)
    return (hidden_res + projected).astype(bf16)


def solution(mesh):
    names = mesh.axis_names
    spread, wide = mesh.shape[names[0]], mesh.shape[names[1]]
    side = GROUP if spread % GROUP == 0 else 1
    along = GROUP if spread % (side * GROUP) == 0 else 1
    outer = spread // (side * along)
    fine = Mesh(mesh.devices.reshape(outer, along, side, wide), ("o", "a", "b", "t"))
    sp = ("o", "a", "b")
    both = P(sp, "t")
    every = P(sp + ("t",), None)
    return jax.shard_map(
        body,
        mesh=fine,
        in_specs=(
            both, both, both, both, both, both,
            P("t"), P("t"), P("t", None),
            every, P(),
            both, both, P(None, "t"), P("t", sp),
        ),
        out_specs=every,
        check_vma=False,
    )
```

```python
import functools

import jax
import jax.numpy as jnp
from jax import lax
from jax.experimental import pallas as pl
from jax.experimental.pallas import tpu as pltpu
from jax.sharding import Mesh, PartitionSpec as P

WIDTH = 64
GROUP = 4
group_eps = 0.00064
norm_eps = 1e-06
f32, bf16 = jnp.float32, jnp.bfloat16
NN, NT, TN = ((1,), (0,)), ((1,), (1,)), ((0,), (0,))


def split(a):
    high = a.astype(bf16)
    return high, (a - high.astype(f32)).astype(bf16)


def dot(a, b, dims=NN):
    return lax.dot_general(a, b, (dims, ((), ())), preferred_element_type=f32)


def dot3(a, b, dims=NN):
    (ah, al), (bh, bl) = a, b
    return dot(ah, bh, dims) + (dot(ah, bl, dims) + dot(al, bh, dims))


MESH = pl.DeviceIdType.MESH


def others(axis):
    size, me = lax.axis_size(axis), lax.axis_index(axis)
    return [(lax.rem(me + d, size), lax.rem(me + size - d, size)) for d in range(1, size)]


def peers(kinds):
    found = []
    for kind in kinds:
        if kind[0] in ("oa", "ob"):
            found += joint_peers(kind[0][1])[0]
        else:
            found += [{kind[0]: to} for to, _ in others(kind[0])]
    return found


def joint_peers(inner):
    count, size = lax.axis_size("o") * lax.axis_size(inner), lax.axis_size(inner)
    me = lax.axis_index("o") * size + lax.axis_index(inner)
    to, come = [], []
    for d in range(1, count):
        there = lax.rem(me + d, count)
        to.append({"o": there // size, inner: lax.rem(there, size)})
        come.append(lax.rem(me + count - d, count))
    return to, come, me


def greet(kinds):
    barrier = pltpu.get_barrier_semaphore()
    who = peers(kinds)
    for device in who:
        pl.semaphore_signal(barrier, inc=1, device_id=device, device_id_type=MESH)
    pl.semaphore_wait(barrier, len(who))


def remote(src, dst, send, recv, device):
    return pltpu.make_async_remote_copy(
        src_ref=src, dst_ref=dst, send_sem=send, recv_sem=recv, device_id=device, device_id_type=MESH
    )


def exchange(sources, targets, sends, recvs, local, step):
    me = lax.axis_index("a")
    mine = joint_peers("b")[2]
    for n, (src, whole) in enumerate(zip(sources, targets)):
        dst = whole.at[mine]
        own = pltpu.make_async_copy(src.at[me], dst.at[me], local.at[n])
        if step == "start":
            own.start()
        for d, (to, come) in enumerate(others("a")):
            out = remote(src.at[to], dst.at[me], sends.at[n, d], recvs.at[n, me], {"a": to})
            if step == "start":
                out.start()
            elif step == n:
                out.wait_send()
                remote(src.at[to], dst.at[come], sends.at[n, d], recvs.at[n, come], {"a": to}).wait_recv()
        if step == n:
            own.wait()


def spread_out(whole, sends, recvs, begin):
    devices, origins, mine = joint_peers("b")
    for d, (device, come) in enumerate(zip(devices, origins)):
        out = remote(whole.at[mine], whole.at[mine], sends.at[d], recvs.at[mine], device)
        if begin:
            out.start()
        else:
            out.wait_send()
            remote(whole.at[mine], whole.at[come], sends.at[d], recvs.at[come], device).wait_recv()


def chunk_kernel(r_ref, k_ref, v_ref, x_ref, l_ref, gate, up, down, q_ref, o_ref, m_ref, gate_out, up_out, down_out, sends, recvs, local, wide_s, wide_r):
    swap = functools.partial(exchange, (gate, up, down), (gate_out, up_out, down_out), sends, recvs, local)

    @pl.when(pl.program_id(0) == 0)
    def _():
        greet([("a",), ("ob",)])
        swap("start")

    @pl.when(pl.program_id(0) == pl.num_programs(0) - 1)
    def _():
        swap(0)
        spread_out(gate_out, wide_s, wide_r, True)

    tokens, lanes = r_ref.shape
    row = lax.broadcasted_iota(jnp.int32, (tokens, tokens), 0)
    col = lax.broadcasted_iota(jnp.int32, (tokens, tokens), 1)
    log_decay = -jax.nn.sigmoid(x_ref[...]) * jnp.exp(jnp.asarray(-0.5, f32))
    ones = (row >= col).astype(bf16)
    d0, rest = split(log_decay)[0], log_decay
    rest = log_decay - d0.astype(f32)
    d1, d2 = split(rest)
    running = dot(ones, d0) + (dot(ones, d1) + dot(ones, d2))
    decay = jnp.exp(running)
    before = jnp.exp(running - log_decay)
    inverse = jnp.exp(-running)
    rate = jax.nn.sigmoid(l_ref[...])
    r_all, k_all, v_all = (a[...].astype(f32) for a in (r_ref, k_ref, v_ref))
    k_hat_all = k_all * inverse
    r_hat_all = r_all * decay
    for head in range(lanes // WIDTH):
        cut = slice(head * WIDTH, (head + 1) * WIDTH)
        k = k_all[:, cut]
        length = jnp.sqrt(jnp.sum(k * k, axis=-1, keepdims=True))
        unit = k / jnp.maximum(length, 1.0)
        a_hat = -unit * before[:, cut]
        b_hat = unit * rate[:, cut] * inverse[:, cut]
        k_hat, r_hat = k_hat_all[:, cut], r_hat_all[:, cut]
        v = v_ref[:, cut]
        bk = split(jnp.concatenate([b_hat, k_hat], axis=0))
        both = dot3(split(jnp.concatenate([a_hat, r_hat], axis=0)), bk, NT)
        erase = jnp.where(row > col, both[:tokens, :tokens], 0.0)
        write = jnp.where(row > col, both[:tokens, tokens:], 0.0)
        out_erase = jnp.where(row >= col, both[tokens:, :tokens], 0.0)
        out_write = jnp.where(row >= col, both[tokens:, tokens:], 0.0)
        solved = (row == col).astype(f32)
        block = 1
        while block < tokens:
            off = (row // block == col // block + 1) & (row // (2 * block) == col // (2 * block))
            part = jnp.where(off, erase, 0.0)
            if block == 1:
                solved = solved + part
            else:
                pieces = split(solved)
                solved = solved + dot3(split(dot3(pieces, split(part))), pieces)
            block *= 2
        wh, wl = split(write)
        seen = jnp.concatenate([a_hat, dot(wh, v) + dot(wl, v)], axis=1)
        kept = dot3(split(solved), split(seen))
        kept_pieces = split(kept)
        oh, ol = split(out_write)
        out = dot3(split(out_erase), kept_pieces) + jnp.concatenate(
            [r_hat, dot(oh, v) + dot(ol, v)], axis=1
        )
        q_ref[:, cut] = out[:, :WIDTH]
        o_ref[:, cut] = out[:, WIDTH:]
        moved = dot3(kept_pieces, tuple(p[:tokens] for p in bk), TN)
        kh, kl = (p[tokens:] for p in bk)
        stored = dot(v, kh, TN) + dot(v, kl, TN)
        eye = (row == col)[:WIDTH, :WIDTH].astype(f32)
        last = decay[tokens - 1 :, cut]
        m_ref[head] = jnp.concatenate(
            [(moved[:WIDTH] + eye) * last, (moved[WIDTH:] + stored) * last], axis=1
        ).astype(bf16)

    @pl.when(pl.program_id(0) == pl.num_programs(0) - 1)
    def _():
        swap(1)
        swap(2)
        spread_out(gate_out, wide_s, wide_r, False)


def chunk(r, k, v, x, l, gate, up, down):
    tokens, channels = r.shape
    pair = 2 * WIDTH
    heads = channels // WIDTH
    size = gate.shape[0]
    side = lax.axis_size("o") * lax.axis_size("b")
    block = pl.BlockSpec((tokens, pair), lambda i: (0, i))
    hbm = pl.BlockSpec(memory_space=pltpu.HBM)
    return pl.pallas_call(
        chunk_kernel,
        grid=(channels // pair,),
        out_shape=(
            jax.ShapeDtypeStruct((tokens, channels), f32),
            jax.ShapeDtypeStruct((tokens, channels), f32),
            jax.ShapeDtypeStruct((heads, WIDTH, pair), bf16),
        )
        + tuple(jax.ShapeDtypeStruct((side,) + w.shape, bf16) for w in (gate, up, down)),
        in_specs=[block] * 5 + [hbm] * 3,
        out_specs=(block, block, pl.BlockSpec((2, WIDTH, pair), lambda i: (i, 0, 0)), hbm, hbm, hbm),
        scratch_shapes=[
            pltpu.SemaphoreType.DMA((3, size)),
            pltpu.SemaphoreType.DMA((3, size)),
            pltpu.SemaphoreType.DMA((3,)),
            pltpu.SemaphoreType.DMA((side,)),
            pltpu.SemaphoreType.DMA((side,)),
        ],
        compiler_params=pltpu.CompilerParams(collective_id=0, has_side_effects=True),
        cost_estimate=pl.CostEstimate(
            flops=heads * 200_000_000, bytes_accessed=tokens * channels * 22, transcendentals=0
        ),
        name="chunk",
    )(r, k, v, x, l, gate, up, down)


def finish_kernel(
    m_ref, q_ref, o_ref, r_ref, k_ref, v_ref, g_ref, e_ref, s_ref, w_ref, skip_ref, gain_ref, up_in, down_in,
    rows_ref, res_ref, up_ref, down_ref,
    near, total, far, mixed, partial, parts, near_s, near_r, far_s, far_r, part_s, part_r, row_s, row_r, pass_s, wide_s, wide_r,
):
    heads = m_ref.shape[0]
    side, across = lax.axis_size("b"), far.shape[0]
    b, a, t = lax.axis_index("b"), lax.axis_index("a"), lax.axis_index("t")
    wide = lax.axis_size("t")
    greet([("ob",), ("oa",), ("t",)])

    sent = []
    for d, (to, come) in enumerate(others("b")):
        copy = remote(m_ref, near.at[b], near_s.at[d], near_r.at[b], {"b": to})
        copy.start()
        sent.append(copy)
    for n, whole in enumerate((up_ref, down_ref)):
        spread_out(whole, wide_s.at[n], wide_r.at[n], True)
    for to, come in others("b"):
        remote(m_ref, near.at[come], near_s.at[0], near_r.at[come], {"b": to}).wait_recv()
    near[b] = m_ref[...]
    eye = (
        lax.broadcasted_iota(jnp.int32, (2 * WIDTH, WIDTH), 0)
        == lax.broadcasted_iota(jnp.int32, (2 * WIDTH, WIDTH), 1)
    ).astype(f32)
    befores = [eye] * heads
    for head in range(heads):
        running = None
        for i in range(side):
            joined = near[i, head]
            move, add = joined[:, :WIDTH], joined[:, WIDTH:]
            if running is None:
                running = jnp.concatenate([move, add], axis=0).astype(f32)
            else:
                befores[head] = jnp.where(b == i, running, befores[head])
                high, low = split(running)
                running = dot(high, move) + dot(low, move)
                running = running + jnp.concatenate(
                    [jnp.zeros((WIDTH, WIDTH), f32), add.astype(f32)], axis=0
                )
        total[head] = jnp.concatenate([running[:WIDTH], running[WIDTH:]], axis=1).astype(bf16)

    to_outer, come_outer, outer = joint_peers("a")
    for d, device in enumerate(to_outer):
        copy = remote(total, far.at[outer], far_s.at[d], far_r.at[outer], device)
        copy.start()
        sent.append(copy)
    for come, device in zip(come_outer, to_outer):
        remote(total, far.at[come], far_s.at[0], far_r.at[come], device).wait_recv()
    far[outer] = total[...]
    for head in range(heads):
        state = jnp.zeros((WIDTH, WIDTH), f32)
        for i in range(across - 1):
            joined = far[i, head]
            high, low = split(state)
            following = dot(high, joined[:, :WIDTH]) + dot(low, joined[:, :WIDTH])
            state = jnp.where(i < outer, following + joined[:, WIDTH:].astype(f32), state)
        state = dot3(split(state), split(befores[head][:WIDTH])) + befores[head][WIDTH:]
        cut = slice(head * WIDTH, (head + 1) * WIDTH)
        o = o_ref[:, cut] + dot3(split(q_ref[:, cut]), split(state), NT)
        centred = o - jnp.mean(o, axis=-1, keepdims=True)
        scaled = centred * lax.rsqrt(jnp.mean(centred * centred, axis=-1, keepdims=True) + group_eps)
        r, k, v, g = (x[:, cut].astype(f32) for x in (r_ref, k_ref, v_ref, g_ref))
        bonus = jnp.sum(r * k * e_ref[:, cut], axis=-1, keepdims=True) * v
        mixed[:, cut] = ((scaled * s_ref[:, cut] + bonus) * g).astype(bf16)

    own = skip_ref.shape[0]
    product = dot(mixed[...], w_ref[...]).astype(bf16)
    for n in range(wide):
        partial[n] = product[n * own : (n + 1) * own]
    for d, (to, come) in enumerate(others("t")):
        copy = remote(partial.at[to], parts.at[t], part_s.at[d], part_r.at[t], {"t": to})
        copy.start()
        sent.append(copy)
    for to, come in others("t"):
        remote(partial.at[to], parts.at[come], part_s.at[0], part_r.at[come], {"t": to}).wait_recv()
    parts[t] = partial[t]
    hidden_res = skip_ref[...].astype(f32)
    attended = parts[0].astype(f32)
    for n in range(1, wide):
        attended = attended + parts[n].astype(f32)
    hidden_res = hidden_res + attended
    res_ref[...] = hidden_res
    normed = (
        hidden_res
        * lax.rsqrt(jnp.mean(hidden_res * hidden_res, axis=-1, keepdims=True) + norm_eps)
        * gain_ref[...]
    )
    normed = normed.astype(bf16)
    outers, along = lax.axis_size("o"), lax.axis_size("a")
    piece = normed.shape[1] // (outers * along * side)
    starts = [((i * along + j) * side + n) * piece for i in range(outers) for n in range(side) for j in range(along)]
    rows_ref[a, t] = jnp.concatenate([normed[:, at : at + piece] for at in starts], axis=1)

    def give(slot, send, device):
        copy = remote(rows_ref.at[slot, t], rows_ref.at[slot, t], send, row_r.at[slot, t], device)
        copy.start()
        sent.append(copy)

    for d, (to, come) in enumerate(others("a")):
        give(a, row_s.at[d], {"a": to})
    for d, (to, come) in enumerate(others("t")):
        give(a, pass_s.at[0, d], {"t": to})
    for d, (to, come) in enumerate(others("a")):
        mine = rows_ref.at[come, t]
        remote(mine, mine, row_s.at[0], row_r.at[come, t], {"a": to}).wait_recv()
        for f, (fro, _) in enumerate(others("t")):
            give(come, pass_s.at[d + 1, f], {"t": fro})
    for i in range(lax.axis_size("a")):
        for to, come in others("t"):
            theirs = rows_ref.at[i, come]
            remote(theirs, theirs, row_s.at[0], row_r.at[i, come], {"t": to}).wait_recv()
    for copy in sent:
        copy.wait_send()
    for n, whole in enumerate((up_ref, down_ref)):
        spread_out(whole, wide_s.at[n], wide_r.at[n], False)


def finish(m, q, o, r, k, v, g, extra, scale, weights, skip, gain, up, down):
    tokens, channels = r.shape
    own, model = skip.shape
    side, along, wide = (lax.axis_size(x) for x in ("b", "a", "t"))
    across = lax.axis_size("o") * along
    vmem = pl.BlockSpec(memory_space=pltpu.VMEM)
    hbm = pl.BlockSpec(memory_space=pltpu.HBM)
    plane = up.shape[0]
    dma = pltpu.SemaphoreType.DMA
    return pl.pallas_call(
        finish_kernel,
        out_shape=(
            jax.ShapeDtypeStruct((along, wide, own, model), bf16),
            jax.ShapeDtypeStruct((own, model), f32),
            jax.ShapeDtypeStruct(up.shape, bf16),
            jax.ShapeDtypeStruct(down.shape, bf16),
        ),
        in_specs=[vmem] * 12 + [hbm] * 2,
        out_specs=(vmem, vmem, hbm, hbm),
        input_output_aliases={12: 2, 13: 3},
        scratch_shapes=[
            pltpu.VMEM((side,) + m.shape, bf16),
            pltpu.VMEM(m.shape, bf16),
            pltpu.VMEM((across,) + m.shape, bf16),
            pltpu.VMEM((tokens, channels), bf16),
            pltpu.VMEM((wide, own, model), bf16),
            pltpu.VMEM((wide, own, model), bf16),
            dma((side,)), dma((side,)), dma((across,)), dma((across,)),
            dma((wide,)), dma((wide,)), dma((along,)), dma((along, wide)), dma((along, wide)),
            dma((2, plane)), dma((2, plane)),
        ],
        compiler_params=pltpu.CompilerParams(collective_id=1, has_side_effects=True),
        cost_estimate=pl.CostEstimate(
            flops=20_000_000_000, bytes_accessed=4_000_000, transcendentals=0
        ),
        name="finish",
    )(m, q, o, r, k, v, g, extra[None], scale[None], weights, skip, gain[None], up, down)


def body(
    r, k, v, x, l, g, extra, scale, exit_weights, skip, gain, gate_w, up_w, taps_w, down_w
):
    tokens = r.shape[0]
    along, side = lax.axis_size("a"), lax.axis_size("b")
    outer = lax.axis_size("o")
    piece = gate_w.shape[0]
    units = gate_w.shape[1] // along

    def by_owner(w):
        return jnp.moveaxis(w.reshape(piece, along, units), 1, 0)

    q, o, m, gate_full, up_part, down_part = chunk(
        r, k, v, x, l, by_owner(gate_w), by_owner(up_w), down_w.reshape(along, units, piece)
    )
    rows, hidden_res, up_full, down_full = finish(
        m, q, o, r, k, v, g, extra, scale, exit_weights, skip, gain, up_part, down_part
    )
    rows = rows.reshape(along * tokens, -1)
    model = rows.shape[1]
    gate_full, up_full = gate_full.reshape(model, units), up_full.reshape(model, units)
    gate_pre = jnp.dot(rows, gate_full, preferred_element_type=f32).astype(bf16)
    gate_pre = gate_pre.reshape(along, tokens, units)
    reach = taps_w.shape[0] - 1
    tail = gate_pre[:, tokens - reach :]
    tail = lax.ppermute(tail, "b", [(i, (i + 1) % side) for i in range(side)])
    if outer > 1:
        first = lax.ppermute(tail[-1:], "o", [(i, i + 1) for i in range(outer - 1)])
    else:
        first = jnp.zeros_like(tail[:1])
    later = jnp.concatenate([first, tail[:-1]], axis=0)
    tail = jnp.where(lax.axis_index("b") == 0, later, tail)
    up_out = jnp.dot(rows, up_full, preferred_element_type=f32).astype(bf16)
    own_taps = lax.dynamic_slice_in_dim(taps_w, lax.axis_index("a") * units, units, 1)
    extended = jnp.concatenate([tail, gate_pre], axis=1).astype(f32)
    conv_out = jnp.zeros(gate_pre.shape, f32)
    for tap in range(reach + 1):
        conv_out = conv_out + own_taps[tap] * extended[:, tap : tap + tokens]
    hidden = (jax.nn.silu(conv_out).reshape(up_out.shape) * up_out.astype(f32)).astype(bf16)
    down_full = jnp.moveaxis(down_full.reshape(outer, side, along, units, piece), 3, 0)
    down_full = jnp.swapaxes(down_full, 2, 3).reshape(units, model)
    projected = lax.psum_scatter(
        jnp.dot(hidden, down_full, preferred_element_type=f32).astype(bf16),
        ("a", "t"),
        scatter_dimension=0,
        tiled=True,
    ).astype(f32)
    return (hidden_res + projected).astype(bf16)


def solution(mesh):
    names = mesh.axis_names
    spread, wide = mesh.shape[names[0]], mesh.shape[names[1]]
    side = GROUP if spread % GROUP == 0 else 1
    along = GROUP if spread % (side * GROUP) == 0 else 1
    outer = spread // (side * along)
    fine = Mesh(mesh.devices.reshape(outer, along, side, wide), ("o", "a", "b", "t"))
    sp = ("o", "a", "b")
    both = P(sp, "t")
    every = P(sp + ("t",), None)
    return jax.shard_map(
        body,
        mesh=fine,
        in_specs=(
            both, both, both, both, both, both,
            P("t"), P("t"), P("t", None),
            every, P(),
            both, both, P(None, "t"), P("t", sp),
        ),
        out_specs=every,
        check_vma=False,
    )
```
